32 devices in a mesh: kv: 8 (over z, y), tp: 4 (over x, core).
Axes of the slice: x: 2, y: 2, z: 4, core: 2. Of those that a mesh axis runs over, the one named last changes fastest.
Arguments:
- hidden_vectors: bfloat16 [64, 2048], P(None, 'kv'), may hold values from -24 to 24
- input_norm_gain: float32 [2048], P('kv'), may hold values from 0.1 to 1.9
- gate_matrix: bfloat16 [2048, 4096], P('kv', 'tp'), may hold values from -0.125 to 0.125
- value_matrix: bfloat16 [2048, 4096], P('kv', 'tp'), may hold values from -0.125 to 0.125
- write_matrix: bfloat16 [2048, 2048], P('kv', 'tp'), may hold values from -0.125 to 0.125
- read_matrix: bfloat16 [2048, 2048], P('kv', 'tp'), may hold values from -0.125 to 0.125
- step_matrix: bfloat16 [2048, 64], P('kv', 'tp'), may hold values from -0.125 to 0.125
- raw_value_rows: bfloat16 [16, 7, 4096], P('kv', None, 'tp'), may hold values from -6 to 6
- raw_write_rows: bfloat16 [16, 7, 2048], P('kv', None, 'tp'), may hold values from -6 to 6
- raw_read_rows: bfloat16 [16, 7, 2048], P('kv', None, 'tp'), may hold values from -6 to 6
- value_filter_taps: bfloat16 [4, 4096], P(None, 'tp'), may hold values from -3 to 3
- write_filter_taps: bfloat16 [4, 2048], P(None, 'tp'), may hold values from -3 to 3
- read_filter_taps: bfloat16 [4, 2048], P(None, 'tp'), may hold values from -3 to 3
- step_size_bias: float32 [64], P('tp'), may hold values from -3 to 0
- rate_logarithm: float32 [64], P('tp'), may hold values from -4 to 0.5
- direct_path_gain: float32 [64], P('tp'), may hold values from 0.1 to 1.9
- prior_step_preact: float32 [16, 4, 64], P('kv', None, 'tp'), may hold values from -6 to 6
- extra_log_decay: float32 [16, 8, 64], P('kv', None, 'tp'), may hold values from -0.7 to 0, as said below
- accepted: int32 [16], P('kv'), may hold values from 0 to 4
- prior_state: float32 [16, 64, 64, 128], P('kv', 'tp'), may hold values from -6 to 6
- group_norm_gain: float32 [4096], P('tp'), may hold values from 0.1 to 1.9
- output_matrix: bfloat16 [4096, 2048], P('tp', 'kv'), may hold values from -0.09375 to 0.09375
Outputs:
- mixer_out: bfloat16 [64, 2048], P('tp', 'kv')
- resumed_state: float32 [16, 64, 64, 128], P('kv', 'tp')
The draws below stay inside these ranges and needn't reach their ends.
Inputs may be any that keep to these rules, and one draw needn't show every extreme that they name: `extra_log_decay`: zero at most positions.
All inputs are finite; a program needn't handle non-finite values.
Results may differ from the reference program's by a relative error of at most 0.0095.
Values may be sent and summed in bfloat16 or wider, within the bound.
A program may use at most 64 MiB of HBM per device.

```python
import math
import jax
import jax.numpy as jnp
from jax import lax

D = 2048
HEADS = 64
HEAD_DIM = 64
GROUPS = 16
STATE = 128
TAPS = 4
DRAFT_TOKENS = 4
INNER = 4096
SEQS = 16
TOKENS = 64
N_TP = 4


def draw_hidden_vectors(key, part):
    normal_base = jax.random.normal(jax.random.fold_in(key, 11), (TOKENS, D), jnp.float32)
    column_scale = jnp.exp(jnp.arange(D, dtype=jnp.float32) * (math.log(4.0) / D)) * 0.5
    values = normal_base * column_scale
    return jnp.clip(values, -24.0, 24.0).astype(jnp.bfloat16)


def draw_extra_log_decay(key, part):
    chosen = jax.random.uniform(jax.random.fold_in(key, 21), (SEQS, 2 * DRAFT_TOKENS, HEADS)) < 0.15
    losses = jnp.log(jax.random.uniform(jax.random.fold_in(key, 22), (SEQS, 2 * DRAFT_TOKENS, HEADS), minval=0.5, maxval=0.8))
    return jnp.where(chosen, losses, 0.0).astype(jnp.float32)


def set_ends(drawn, key, smallest, top_value):
    shape = drawn.shape
    index_at = [jax.random.randint(jax.random.fold_in(key, axis), (), 0, shape[axis]) for axis in range(len(shape))]
    drawn = drawn.at[tuple(index_at)].set(smallest)
    longest = shape.index(max(shape))
    index_at[longest] = (index_at[longest] + 1) % shape[longest]
    return drawn.at[tuple(index_at)].set(top_value)


def shard_levels(stream_key, extent, shards, low, largest):
    def one(dim, blocks):
        heights = jax.random.uniform(jax.random.fold_in(jax.random.fold_in(stream_key, 6), dim), (blocks,), jnp.float32, low / len(shards), largest / len(shards))
        return jnp.repeat(jnp.exp(heights), extent[dim] // blocks).reshape((-1,) + (1,) * (len(extent) - dim - 1))

    gain = one(*shards[0])
    for cut in shards[1:]:
        gain = gain * one(*cut)
    return gain


def normal_values(stream_key, extent, spread, reach, pieces=(), kind=jnp.bfloat16):
    values = jax.random.normal(stream_key, extent, jnp.float32) * spread
    if len(pieces) > 0:
        values = shard_levels(stream_key, extent, pieces, -0.22, 0.18) * values
    return jnp.clip(values, min=-reach, max=reach).astype(kind)


def setup_inputs(seed: int = 0) -> dict:
    key_of = jax.random.split(jax.random.key(seed), 23)
    hidden_vectors = draw_hidden_vectors(jax.random.fold_in(key_of[22], 71), 0)
    input_norm_gain = jnp.clip(1.0 + 0.18 * jax.random.normal(key_of[1], (D,), jnp.float32), 0.1, 1.9)
    gate_matrix = normal_values(key_of[2], (D, INNER), D ** -0.5, 0.125, ((0, 8), (1, 4)))
    value_matrix = normal_values(key_of[3], (D, INNER), D ** -0.5, 0.125, ((0, 8), (1, 4)))
    write_matrix = normal_values(key_of[4], (D, GROUPS * STATE), D ** -0.5, 0.125, ((0, 8), (1, 4)))
    read_matrix = normal_values(key_of[5], (D, GROUPS * STATE), D ** -0.5, 0.125, ((0, 8), (1, 4)))
    step_matrix = normal_values(key_of[6], (D, HEADS), D ** -0.5, 0.125, ((0, 8), (1, 4)))
    raw_value_rows = normal_values(key_of[7], (SEQS, TAPS - 1 + DRAFT_TOKENS, INNER), 1.0, 6.0, ((0, 8), (2, 4)))
    raw_write_rows = normal_values(key_of[8], (SEQS, TAPS - 1 + DRAFT_TOKENS, GROUPS * STATE), 1.0, 6.0, ((0, 8), (2, 4)))
    raw_read_rows = normal_values(key_of[9], (SEQS, TAPS - 1 + DRAFT_TOKENS, GROUPS * STATE), 1.0, 6.0, ((0, 8), (2, 4)))
    value_filter_taps = normal_values(key_of[10], (TAPS, INNER), TAPS ** -0.5, 3.0, ((1, 4),))
    write_filter_taps = normal_values(key_of[11], (TAPS, GROUPS * STATE), TAPS ** -0.5, 3.0, ((1, 4),))
    read_filter_taps = normal_values(key_of[12], (TAPS, GROUPS * STATE), TAPS ** -0.5, 3.0, ((1, 4),))
    step_size_bias = jnp.clip(-3.0 + 3.0 * jax.random.uniform(key_of[13], (HEADS,), jnp.float32) ** shard_levels(key_of[13], (HEADS,), ((0, 4),), -0.2, 0.2), -3.0, 0.0)
    rate_logarithm = jnp.clip(-4.0 + 4.5 * jax.random.uniform(key_of[14], (HEADS,), jnp.float32) ** shard_levels(key_of[14], (HEADS,), ((0, 4),), -0.2, 0.2), -4.0, 0.5)
    direct_path_gain = jnp.clip(1.0 + 0.18 * jax.random.normal(key_of[15], (HEADS,), jnp.float32), 0.1, 1.9)
    prior_step_preact = normal_values(key_of[16], (SEQS, DRAFT_TOKENS, HEADS), 1.0, 6.0, ((0, 8), (2, 4)), jnp.float32)
    extra_log_decay = draw_extra_log_decay(jax.random.fold_in(key_of[22], 71), 0)
    accepted = set_ends(jax.random.randint(key_of[18], (SEQS,), 0, DRAFT_TOKENS + 1), jax.random.fold_in(key_of[18], 1), 0, DRAFT_TOKENS).astype(jnp.int32)
    prior_state = normal_values(key_of[19], (SEQS, HEADS, HEAD_DIM, STATE), 1.0, 6.0, ((0, 8), (1, 4)), jnp.float32)
    group_norm_gain = jnp.clip(1.0 + 0.18 * jax.random.normal(key_of[20], (INNER,), jnp.float32), 0.1, 1.9)
    output_matrix = normal_values(key_of[21], (INNER, D), INNER ** -0.5, 0.09375, ((0, 4), (1, 8)))
    return dict(hidden_vectors=hidden_vectors, input_norm_gain=input_norm_gain, gate_matrix=gate_matrix, value_matrix=value_matrix, write_matrix=write_matrix, read_matrix=read_matrix, step_matrix=step_matrix, raw_value_rows=raw_value_rows, raw_write_rows=raw_write_rows, raw_read_rows=raw_read_rows, value_filter_taps=value_filter_taps, write_filter_taps=write_filter_taps, read_filter_taps=read_filter_taps, step_size_bias=step_size_bias, rate_logarithm=rate_logarithm, direct_path_gain=direct_path_gain, prior_step_preact=prior_step_preact, extra_log_decay=extra_log_decay, accepted=accepted, prior_state=prior_state, group_norm_gain=group_norm_gain, output_matrix=output_matrix)


epsilon = 1e-06
highest = lax.Precision.HIGHEST

def conv_rows(row_block, taps):
    length_rows = row_block.shape[1] - (TAPS - 1)
    result = jnp.zeros((row_block.shape[0], length_rows, row_block.shape[2]), jnp.float32)
    for tap_index in range(TAPS):
        result = result + row_block[:, tap_index:tap_index + length_rows].astype(jnp.float32) * taps[tap_index].astype(jnp.float32)
    return jax.nn.silu(result)

def resume_state(start_state, values, writes, head_step_size, decay_logarithm, accepted):
    live_mask = (jnp.arange(values.shape[1])[None, :] < accepted[:, None]).astype(jnp.float32)
    kept_decay = decay_logarithm * live_mask[:, :, None]
    total_decay = lax.optimization_barrier(jnp.sum(kept_decay, axis=1))
    tail_decay = total_decay[:, None, :] - jnp.cumsum(kept_decay, axis=1)
    coefficient = live_mask[:, :, None] * jnp.exp(tail_decay) * head_step_size
    added = jnp.einsum('skh,skhp,skhn->shpn', coefficient, values, writes, precision=highest)
    return jnp.exp(total_decay)[:, :, None, None] * start_state + added

def dual_block(values, writes, reads, head_step_size, decay_logarithm, direct_path_gain, start_state):
    cumulative = jnp.cumsum(decay_logarithm, axis=1)
    carried = jnp.exp(cumulative)[..., None] * jnp.einsum('skhn,shpn->skhp', reads, start_state, precision=highest)
    order = jnp.arange(cumulative.shape[1])
    causal = order[:, None] >= order[None, :]
    difference = cumulative[:, :, None, :] - cumulative[:, None, :, :]
    decay_weight = jnp.where(causal[None, :, :, None], jnp.exp(jnp.minimum(difference, 0.0)), 0.0)
    inner_terms = jnp.einsum('sthn,suhn->stuh', reads, writes, precision=highest)
    within = jnp.einsum('stuh,suh,suhp->sthp', inner_terms * decay_weight, head_step_size, values, precision=highest)
    return carried + within + direct_path_gain[None, None, :, None] * values

def mixer_kernel_body(output_gate, fresh_values, fresh_writes, fresh_reads, step_preact, raw_value_rows, raw_write_rows, raw_read_rows, value_filter_taps, write_filter_taps, read_filter_taps, step_size_bias, rate_logarithm, direct_path_gain, prior_step_preact, extra_log_decay, accepted, prior_state, group_norm_gain):
    seq_count = raw_value_rows.shape[0]
    head_count = step_preact.shape[2]
    group_count = fresh_writes.shape[2] // STATE
    per_group = head_count // group_count
    window = accepted[:, None] + jnp.arange(TAPS - 1, dtype=jnp.int32)[None, :]

    def current(row_block, new_rows, taps):
        earlier = jnp.take_along_axis(row_block, window[:, :, None], axis=1)
        return conv_rows(jnp.concatenate([earlier, new_rows], axis=1), taps)
    conv_values = current(raw_value_rows, fresh_values, value_filter_taps).reshape(seq_count, DRAFT_TOKENS, head_count, HEAD_DIM)
    conv_writes = current(raw_write_rows, fresh_writes, write_filter_taps).reshape(seq_count, DRAFT_TOKENS, group_count, STATE)
    conv_reads = current(raw_read_rows, fresh_reads, read_filter_taps).reshape(seq_count, DRAFT_TOKENS, group_count, STATE)
    last_values = conv_rows(raw_value_rows, value_filter_taps).reshape(seq_count, DRAFT_TOKENS, head_count, HEAD_DIM)
    last_writes = conv_rows(raw_write_rows, write_filter_taps).reshape(seq_count, DRAFT_TOKENS, group_count, STATE)
    head_decay_rate = jnp.exp(rate_logarithm)
    head_step_size = jax.nn.softplus(step_preact + step_size_bias)
    decay_logarithm = -head_decay_rate * head_step_size + extra_log_decay[:, DRAFT_TOKENS:]
    prior_step = jax.nn.softplus(prior_step_preact + step_size_bias)
    prior_decay = -head_decay_rate * prior_step + extra_log_decay[:, :DRAFT_TOKENS]
    restored_state = resume_state(prior_state, last_values, jnp.repeat(last_writes, per_group, axis=2), prior_step, prior_decay, accepted)
    mixed_heads = dual_block(conv_values, jnp.repeat(conv_writes, per_group, axis=2), jnp.repeat(conv_reads, per_group, axis=2), head_step_size, decay_logarithm, direct_path_gain, restored_state)
    gated = mixed_heads.reshape(seq_count, DRAFT_TOKENS, -1) * jax.nn.silu(output_gate.astype(jnp.float32))
    group_width = INNER // GROUPS
    grouped = gated.reshape(seq_count, DRAFT_TOKENS, -1, group_width)
    scale = lax.rsqrt(lax.optimization_barrier(jnp.mean(grouped * grouped, axis=-1, keepdims=True)) + epsilon)
    normalized_hidden = (grouped * scale).reshape(seq_count, DRAFT_TOKENS, -1) * group_norm_gain
    return (normalized_hidden.astype(jnp.bfloat16).reshape(seq_count * DRAFT_TOKENS, -1), restored_state)

def reference(hidden_vectors, input_norm_gain, gate_matrix, value_matrix, write_matrix, read_matrix, step_matrix, raw_value_rows, raw_write_rows, raw_read_rows, value_filter_taps, write_filter_taps, read_filter_taps, step_size_bias, rate_logarithm, direct_path_gain, prior_step_preact, extra_log_decay, accepted, prior_state, group_norm_gain, output_matrix):
    floats_in = hidden_vectors.astype(jnp.float32)
    inverse = lax.rsqrt(lax.optimization_barrier(jnp.mean(floats_in * floats_in, axis=1)) + epsilon)[:, None]
    scaled = (floats_in * input_norm_gain).astype(jnp.bfloat16)

    def project(weight):
        return inverse * jnp.dot(scaled, weight, preferred_element_type=jnp.float32)

    def shaped(matrix):
        return matrix.reshape(SEQS, DRAFT_TOKENS, -1)
    output_gate = shaped(project(gate_matrix).astype(jnp.bfloat16))
    fresh_values = shaped(project(value_matrix).astype(jnp.bfloat16))
    fresh_writes = shaped(project(write_matrix).astype(jnp.bfloat16))
    fresh_reads = shaped(project(read_matrix).astype(jnp.bfloat16))
    step_preact = shaped(project(step_matrix))
    normalized_hidden, restored_state = mixer_kernel_body(output_gate, fresh_values, fresh_writes, fresh_reads, step_preact, raw_value_rows, raw_write_rows, raw_read_rows, value_filter_taps, write_filter_taps, read_filter_taps, step_size_bias, rate_logarithm, direct_path_gain, prior_step_preact, extra_log_decay, accepted, prior_state, group_norm_gain)
    block_width = INNER // N_TP
    mixer_out = jnp.zeros((TOKENS, D), jnp.float32)
    for block_index in range(N_TP):
        lower = block_index * block_width
        partial_value = jnp.dot(normalized_hidden[:, lower:lower + block_width], output_matrix[lower:lower + block_width], preferred_element_type=jnp.float32).astype(jnp.bfloat16)
        partial_value = lax.optimization_barrier(partial_value)
        mixer_out = mixer_out + partial_value.astype(jnp.float32)
    return (mixer_out.astype(jnp.bfloat16), restored_state)
```

```python
import functools

import jax
import jax.numpy as jnp
from jax import lax
from jax.experimental import pallas as pl
from jax.experimental.pallas import tpu as pltpu
from jax.sharding import PartitionSpec as P

HEAD_DIM = 64
STATE = 128
TAPS = 4
DRAFT = 4
EPS = 1e-06
F32 = jnp.float32
BF16 = jnp.bfloat16


def iota(shape, dim):
    return lax.broadcasted_iota(jnp.int32, shape, dim)


def silu(x):
    return x / (1.0 + jnp.exp(-x))


def softplus(x):
    return jnp.maximum(x, 0.0) + jnp.log1p(jnp.exp(-jnp.abs(x)))


def dot(a, b, dims=((1,), (0,)), precision=None):
    return lax.dot_general(
        a, b, (dims, ((), ())), preferred_element_type=F32, precision=precision
    )


def split(x):
    high = x.astype(BF16)
    return high, (x - high.astype(F32)).astype(BF16)


def body(nkv, ntp, *refs):
    (
        hid_h, gain_h, gate_h, value_h, write_h, read_h, step_h,
        rawv_h, raww_h, rawr_h, tapv_h, tapw_h, tapr_h,
        bias_h, rate_h, direct_h, prior_h, extra_h, acc_h, state_h, gng_h, outm_h,
        out_ref, res_ref,
        hid, gain, gate, value, write, read, step, rawv, raww, rawr,
        tapv, tapw, tapr, bias, rate, direct, prior, extra, acc, state, gng, outm,
        sbuf, rbuf, saux, raux, gbuf, pbuf, qbuf, s_hi, s_lo,
        load_sem, send_sem, recv_sem, gsend_sem, grecv_sem, psend_sem, precv_sem,
    ) = refs
    me = lax.axis_index("kv")
    my_tp = lax.axis_index("tp")
    rows = sbuf.shape[1]
    seqs = rawv.shape[0]
    tokens, depth = hid.shape
    heads = step.shape[1]
    cv, cw = value.shape[1], write.shape[1]
    groups = cw // STATE
    width = cv // groups
    per_group = heads // groups
    raw_len = rawv.shape[1]
    MESH = pl.DeviceIdType.MESH

    loads = {}
    order = (
        ("hid", hid_h, hid), ("gain", gain_h, gain), ("step", step_h, step),
        ("write", write_h, write), ("read", read_h, read), ("value", value_h, value),
        ("gate", gate_h, gate), ("acc", acc_h, acc), ("rawv", rawv_h, rawv),
        ("raww", raww_h, raww), ("rawr", rawr_h, rawr), ("tapv", tapv_h, tapv),
        ("tapw", tapw_h, tapw), ("tapr", tapr_h, tapr), ("bias", bias_h, bias),
        ("rate", rate_h, rate), ("direct", direct_h, direct), ("prior", prior_h, prior),
        ("extra", extra_h, extra), ("state", state_h, state), ("gng", gng_h, gng),
        ("outm", outm_h, outm),
    )
    for i, (name, src, dst) in enumerate(order):
        loads[name] = pltpu.make_async_copy(src, dst, load_sem.at[i])
        loads[name].start()

    barrier = pltpu.get_barrier_semaphore()
    for off in range(1, nkv):
        pl.semaphore_signal(
            barrier, inc=1, device_id={"kv": lax.rem(me + off, nkv)}, device_id_type=MESH
        )
    for off in range(1, ntp):
        pl.semaphore_signal(
            barrier, inc=1, device_id={"tp": lax.rem(my_tp + off, ntp)}, device_id_type=MESH
        )

    loads["hid"].wait()
    loads["gain"].wait()
    loads["step"].wait()
    floats = hid[...].astype(F32)
    squares = jnp.sum(floats * floats, axis=1, keepdims=True)
    scaled = (floats * gain[...]).astype(BF16)
    saux[:, :, :STATE] = jnp.broadcast_to(squares, (tokens, STATE)).reshape(nkv, rows, STATE)
    saux[:, :, STATE:] = jnp.zeros((nkv, rows, STATE), F32)
    saux[:, :, STATE : STATE + heads] = dot(scaled, step[...]).reshape(nkv, rows, heads)

    sends = []

    def exchange(buffer, target, start, size, part):
        for off in range(1, nkv):
            peer = lax.rem(me + off, nkv)
            if size is None:
                src, dst = buffer.at[peer], target.at[off - 1]
            else:
                src = buffer.at[peer, :, pl.ds(start, size)]
                dst = target.at[off - 1, :, pl.ds(start, size)]
            copy = pltpu.make_async_remote_copy(
                src_ref=src, dst_ref=dst,
                send_sem=send_sem.at[part, off - 1], recv_sem=recv_sem.at[part, off - 1],
                device_id={"kv": peer}, device_id_type=MESH,
            )
            copy.start()
            sends.append((part, copy))

    def project(name, ref, start):
        loads[name].wait()
        size = ref.shape[1]
        part = dot(scaled, ref[...])
        sbuf[:, :, start : start + size] = part.reshape(nkv, rows, size).astype(BF16)

    project("write", write, 0)
    project("read", read, cw)
    pl.semaphore_wait(barrier, nkv - 1 + ntp - 1)
    exchange(saux, raux, 0, None, 0)
    exchange(sbuf, rbuf, 0, 2 * cw, 1)
    project("value", value, 2 * cw)
    exchange(sbuf, rbuf, 2 * cw, cv, 2)
    project("gate", gate, 2 * cw + cv)
    exchange(sbuf, rbuf, 2 * cw + cv, cv, 3)

    for name in (
        "acc", "rawv", "raww", "rawr", "tapv", "tapw", "tapr", "bias", "rate", "direct",
        "prior", "extra",
    ):
        loads[name].wait()
    early = TAPS - 1
    kinds = early + TAPS

    def shifts(ref, count):
        total = None
        for s in range(seqs):
            shape = (count * rows, raw_len)
            index, r = iota(shape, 0), iota(shape, 1)
            kind = lax.div(index, rows)
            within = lax.rem(index, rows)
            t = lax.rem(within, DRAFT)
            here = lax.div(within, DRAFT) == s
            is_early = (kind < early) & (t + kind < early) & (r == acc[s] + t + kind)
            is_last = (kind >= early) & (r == t + kind - early)
            pick = jnp.where(here & (is_early | is_last), 1.0, 0.0).astype(BF16)
            term = dot(pick, ref[s])
            total = term if total is None else total + term
        return total

    def tap(taps, j):
        return taps[j : j + 1, :].astype(F32)

    def early_of(moved, taps):
        return sum(
            moved[j * rows : (j + 1) * rows] * tap(taps, j) for j in range(early)
        )

    def last_of(moved, taps):
        return silu(
            sum(
                moved[(early + j) * rows : (early + j + 1) * rows] * tap(taps, j)
                for j in range(TAPS)
            )
        )

    moved = shifts(rawv, kinds)
    early_v = early_of(moved, tapv)
    last_v = last_of(moved, tapv)
    moved = shifts(raww, kinds)
    early_w = early_of(moved, tapw)
    last_w = last_of(moved, tapw)
    early_r = early_of(shifts(rawr, early), tapr)

    square = (rows, rows)
    ri, ci = iota(square, 0), iota(square, 1)
    same = lax.div(ri, DRAFT) == lax.div(ci, DRAFT)

    def mix(mask, x):
        return dot(jnp.where(mask, 1.0, 0.0), x, precision=lax.Precision.HIGHEST)

    spread = jnp.where(
        lax.div(iota((heads, cv), 1), HEAD_DIM) == iota((heads, cv), 0), 1.0, 0.0
    ).astype(BF16)

    def expand(x):
        high, low = split(x)
        return dot(high, spread) + dot(low, spread)

    head_shape = (rows, heads)
    row_h = iota(head_shape, 0)
    rate_e = jnp.exp(rate[...])
    seq_h = lax.div(row_h, DRAFT)
    accepted = jnp.zeros(head_shape, jnp.int32)
    for s in range(seqs):
        accepted = jnp.where(seq_h == s, acc[s], accepted)
    live = jnp.where(lax.rem(row_h, DRAFT) < accepted, 1.0, 0.0)
    prior_x = jnp.concatenate([prior[s] for s in range(seqs)], axis=0)
    extra_p = jnp.concatenate([extra[s, :DRAFT] for s in range(seqs)], axis=0)
    extra_n = jnp.concatenate([extra[s, DRAFT:] for s in range(seqs)], axis=0)
    prior_step = softplus(prior_x + bias[...])
    kept = live * (extra_p - rate_e * prior_step)
    total_decay = jnp.exp(mix(same, kept))
    tail = mix(same & (ci > ri), kept)
    coefficient = expand(live * jnp.exp(tail) * prior_step)
    direct_e = expand(jnp.broadcast_to(direct[...], head_shape))
    weighted = coefficient * last_v
    row_c = lax.div(iota((rows, width), 0), DRAFT)
    loads["state"].wait()
    for g in range(groups):
        lanes = slice(g * STATE, (g + 1) * STATE)
        for s in range(seqs):
            a = jnp.where(row_c == s, weighted[:, g * width : (g + 1) * width], 0.0)
            added = dot(a, last_w[:, lanes], ((0,), (0,)), lax.Precision.HIGHEST)
            for i in range(per_group):
                h = g * per_group + i
                decay = total_decay[s * DRAFT : s * DRAFT + 1, h : h + 1]
                new = decay * state[s, h] + added[i * HEAD_DIM : (i + 1) * HEAD_DIM]
                res_ref[s, h] = new
                high, low = split(new)
                at = slice(h * HEAD_DIM, (h + 1) * HEAD_DIM)
                s_hi[s, at] = high
                s_lo[s, at] = low

    def arrive(part):
        for p, copy in sends:
            if p == part:
                copy.wait_recv()

    arrive(0)
    aux = saux[me]
    for off in range(1, nkv):
        aux = aux + raux[off - 1]
    inverse = lax.rsqrt(aux[:, :1] * (1.0 / (depth * nkv)) + EPS)
    step_pre = inverse * aux[:, STATE : STATE + heads]
    step_now = softplus(step_pre + bias[...])
    log_decay = extra_n - rate_e * step_now
    cumulative = mix(same & (ci <= ri), log_decay)
    stack = [jnp.exp(cumulative)]
    for d in range(DRAFT):
        if d == 0:
            stack.append(step_now)
        else:
            back = same & (ci == ri - d)
            gap = cumulative - mix(back, cumulative)
            stack.append(jnp.exp(jnp.minimum(gap, 0.0)) * mix(back, step_now))
    wide = expand(jnp.concatenate(stack, axis=0))
    carry_e = wide[:rows]
    coef = [wide[(d + 1) * rows : (d + 2) * rows] for d in range(DRAFT)]

    def summed(start, size):
        total = sbuf[me, :, start : start + size].astype(F32)
        for off in range(1, nkv):
            total = total + rbuf[off - 1, :, start : start + size].astype(F32)
        return (inverse * total).astype(BF16).astype(F32)

    def delayed(x, d):
        if d == 0:
            return x
        keep = lax.rem(iota(x.shape, 0), DRAFT) >= d
        return jnp.where(keep, pltpu.roll(x, d, 0), 0.0)

    def conv(before, new, taps):
        total = before
        for d in range(DRAFT):
            total = total + tap(taps, TAPS - 1 - d) * delayed(new, d)
        return silu(total)

    arrive(1)
    writes = conv(early_w, summed(0, cw), tapw)
    reads = conv(early_r, summed(cw, cw), tapr)
    r_hi, r_lo = split(reads)
    r_both = jnp.concatenate([r_hi, r_lo], axis=0)
    carried = []
    for g in range(groups):
        lanes = slice(g * STATE, (g + 1) * STATE)
        result = None
        for s in range(seqs):
            at = slice(g * width, (g + 1) * width)
            both = dot(r_both[:, lanes], s_hi[s, at], ((1,), (1,)))
            low = dot(r_hi[:, lanes], s_lo[s, at], ((1,), (1,)))
            one = both[:rows] + both[rows:] + low
            result = one if result is None else jnp.where(row_c == s, one, result)
        carried.append(result)
    inner = []
    for d in range(DRAFT):
        product = reads * delayed(writes, d)
        inner.append(
            [
                jnp.sum(product[:, g * STATE : (g + 1) * STATE], axis=1, keepdims=True)
                for g in range(groups)
            ]
        )

    arrive(2)
    values = conv(early_v, summed(2 * cw, cv), tapv)
    moved_values = [delayed(values, d) for d in range(DRAFT)]
    mixed = []
    for g in range(groups):
        at = slice(g * width, (g + 1) * width)
        one = carry_e[:, at] * carried[g] + direct_e[:, at] * values[:, at]
        for d in range(DRAFT):
            one = one + inner[d][g] * coef[d][:, at] * moved_values[d][:, at]
        mixed.append(one)

    arrive(3)
    loads["gng"].wait()
    opened = silu(summed(2 * cw + cv, cv))
    for g in range(groups):
        at = slice(g * width, (g + 1) * width)
        gated = mixed[g] * opened[:, at]
        scale = lax.rsqrt(
            jnp.sum(gated * gated, axis=1, keepdims=True) * (1.0 / width) + EPS
        )
        gbuf[me, :, at] = (gated * scale * gng[:, at]).astype(BF16)

    gathers = []
    for off in range(1, nkv):
        peer = lax.rem(me + off, nkv)
        copy = pltpu.make_async_remote_copy(
            src_ref=gbuf.at[me], dst_ref=gbuf.at[me],
            send_sem=gsend_sem.at[off - 1], recv_sem=grecv_sem.at[off - 1],
            device_id={"kv": peer}, device_id_type=MESH,
        )
        copy.start()
        gathers.append(copy)
    loads["outm"].wait()
    for copy in gathers:
        copy.wait_recv()
    share = tokens // ntp
    normed = gbuf[...].astype(F32).reshape(tokens, cv).astype(BF16)
    partial = dot(normed, outm[...])
    pbuf[...] = partial.reshape(ntp, share, outm.shape[1]).astype(BF16)
    parts = []
    for off in range(1, ntp):
        peer = lax.rem(my_tp + off, ntp)
        copy = pltpu.make_async_remote_copy(
            src_ref=pbuf.at[peer], dst_ref=qbuf.at[off - 1],
            send_sem=psend_sem.at[off - 1], recv_sem=precv_sem.at[off - 1],
            device_id={"tp": peer}, device_id_type=MESH,
        )
        copy.start()
        parts.append(copy)
    total = pbuf[my_tp].astype(F32)
    for off in range(1, ntp):
        parts[off - 1].wait_recv()
        total = total + qbuf[off - 1].astype(F32)
    out_ref[...] = total.astype(BF16)
    for _, copy in sends:
        copy.wait_send()
    for copy in gathers + parts:
        copy.wait_send()


def per_device(nkv, ntp, *args):
    flat = [x.reshape(1, -1) if x.ndim == 1 and x.dtype == F32 else x for x in args]
    tokens = args[0].shape[0]
    rows = tokens // nkv
    gate, value, write, read, step = args[2:7]
    outm = args[21]
    cv, cw = value.shape[1], write.shape[1]
    total = gate.shape[1] + cv + 2 * cw
    state = args[19]
    scratch = []
    for i, x in enumerate(flat):
        space = pltpu.SMEM if i == 18 else pltpu.VMEM
        scratch.append(space(x.shape, x.dtype))
    DMA = pltpu.SemaphoreType.DMA
    scratch += [
        pltpu.VMEM((nkv, rows, total), BF16),
        pltpu.VMEM((nkv - 1, rows, total), BF16),
        pltpu.VMEM((nkv, rows, 2 * STATE), F32),
        pltpu.VMEM((nkv - 1, rows, 2 * STATE), F32),
        pltpu.VMEM((nkv, rows, cv), BF16),
        pltpu.VMEM((ntp, tokens // ntp, outm.shape[1]), BF16),
        pltpu.VMEM((ntp - 1, tokens // ntp, outm.shape[1]), BF16),
        pltpu.VMEM((state.shape[0], cv, STATE), BF16),
        pltpu.VMEM((state.shape[0], cv, STATE), BF16),
        DMA((len(flat),)),
        DMA((4, nkv - 1)),
        DMA((4, nkv - 1)),
        DMA((nkv - 1,)),
        DMA((nkv - 1,)),
        DMA((ntp - 1,)),
        DMA((ntp - 1,)),
    ]
    return pl.pallas_call(
        functools.partial(body, nkv, ntp),
        out_shape=(
            jax.ShapeDtypeStruct((tokens // ntp, outm.shape[1]), BF16),
            jax.ShapeDtypeStruct(state.shape, F32),
        ),
        in_specs=[pl.BlockSpec(memory_space=pl.ANY)] * len(flat),
        out_specs=(
            pl.BlockSpec(memory_space=pltpu.VMEM),
            pl.BlockSpec(memory_space=pltpu.VMEM),
        ),
        scratch_shapes=scratch,
        compiler_params=pltpu.CompilerParams(collective_id=0, has_side_effects=True),
        name="mixer",
    )(*flat)


def solution(mesh):
    placed = (
        P(None, "kv"),
        P("kv"),
        P("kv", "tp"),
        P("kv", "tp"),
        P("kv", "tp"),
        P("kv", "tp"),
        P("kv", "tp"),
        P("kv", None, "tp"),
        P("kv", None, "tp"),
        P("kv", None, "tp"),
        P(None, "tp"),
        P(None, "tp"),
        P(None, "tp"),
        P("tp"),
        P("tp"),
        P("tp"),
        P("kv", None, "tp"),
        P("kv", None, "tp"),
        P("kv"),
        P("kv", "tp", None, None),
        P("tp"),
        P("tp", "kv"),
    )
    return jax.shard_map(
        functools.partial(per_device, mesh.shape["kv"], mesh.shape["tp"]),
        mesh=mesh,
        in_specs=placed,
        out_specs=(P("tp", "kv"), P("kv", "tp", None, None)),
        check_vma=False,
    )
```

```python
import functools

import jax
import jax.numpy as jnp
from jax import lax
from jax.experimental import pallas as pl
from jax.experimental.pallas import tpu as pltpu
from jax.sharding import PartitionSpec as P

HEAD_DIM = 64
STATE = 128
TAPS = 4
DRAFT = 4
EPS = 1e-06
F32 = jnp.float32
BF16 = jnp.bfloat16


def iota(shape, dim):
    return lax.broadcasted_iota(jnp.int32, shape, dim)


def silu(x):
    return x / (1.0 + jnp.exp(-x))


def softplus(x):
    return jnp.maximum(x, 0.0) + jnp.log1p(jnp.exp(-jnp.abs(x)))


def dot(a, b, dims=((1,), (0,)), precision=None):
    return lax.dot_general(
        a, b, (dims, ((), ())), preferred_element_type=F32, precision=precision
    )


def split(x):
    high = x.astype(BF16)
    return high, (x - high.astype(F32)).astype(BF16)


def body(nkv, ntp, *refs):
    (
        hid_h, gain_h, gate_h, value_h, write_h, read_h, step_h,
        rawv_h, raww_h, rawr_h, tapv_h, tapw_h, tapr_h,
        bias_h, rate_h, direct_h, prior_h, extra_h, acc_h, state_h, gng_h, outm_h,
        out_ref, res_ref,
        hid, gain, gate, value, write, read, step, rawv, raww, rawr,
        tapv, tapw, tapr, bias, rate, direct, prior, extra, acc, state, gng, outm,
        sbuf, fbuf, nbuf, xs, xr, saux, faux, naux, xsa, xra,
        gbuf, pbuf, qbuf, s_hi, s_lo,
        load_sem, f_send, f_recv, n_send, n_recv, x_send, x_recv,
        gsend_sem, grecv_sem, psend_sem, precv_sem,
    ) = refs
    me = lax.axis_index("kv")
    my_tp = lax.axis_index("tp")
    chunks, _, rows, _ = sbuf.shape
    inner = nkv // 2
    place = lax.rem(me, inner)
    mine = me - place
    theirs = inner - mine
    seqs = rawv.shape[1]
    tokens, depth = hid.shape
    heads = step.shape[0]
    cv, cw = value.shape[1], write.shape[1]
    groups = cw // STATE
    width = cv // groups
    per_group = heads // groups
    raw_len = rawv.shape[0]
    MESH = pl.DeviceIdType.MESH

    loads = {}
    order = (
        ("hid", hid_h, hid), ("gain", gain_h, gain), ("step", step_h, step),
        ("write", write_h, write), ("read", read_h, read), ("value", value_h, value),
        ("gate", gate_h, gate), ("acc", acc_h, acc), ("rawv", rawv_h, rawv),
        ("raww", raww_h, raww), ("rawr", rawr_h, rawr), ("tapv", tapv_h, tapv),
        ("tapw", tapw_h, tapw), ("tapr", tapr_h, tapr), ("bias", bias_h, bias),
        ("rate", rate_h, rate), ("direct", direct_h, direct), ("prior", prior_h, prior),
        ("extra", extra_h, extra), ("state", state_h, state), ("gng", gng_h, gng),
        ("outm", outm_h, outm),
    )
    for i, (name, src, dst) in enumerate(order):
        loads[name] = pltpu.make_async_copy(src, dst, load_sem.at[i])
        loads[name].start()

    barrier = pltpu.get_barrier_semaphore()
    for off in range(1, nkv):
        pl.semaphore_signal(
            barrier, inc=1, device_id={"kv": lax.rem(me + off, nkv)}, device_id_type=MESH
        )
    for off in range(1, ntp):
        pl.semaphore_signal(
            barrier, inc=1, device_id={"tp": lax.rem(my_tp + off, ntp)}, device_id_type=MESH
        )

    loads["hid"].wait()
    loads["gain"].wait()
    loads["step"].wait()
    floats = hid[...].astype(F32)
    squares = jnp.sum(floats * floats, axis=1, keepdims=True)
    scaled = (floats * gain[...]).astype(BF16)
    saux[...] = jnp.broadcast_to(squares, (tokens, STATE)).reshape(nkv, rows, STATE)
    saux[:, :, :heads] = dot(scaled, step[...], ((1,), (1,))).reshape(nkv, rows, heads)
    wc, vc, gc = cw // chunks, cv // chunks, groups // chunks

    def project(name, ref, start):
        loads[name].wait()
        size = ref.shape[1] // chunks
        part = dot(scaled, ref[...])
        for c in range(chunks):
            piece = part[:, c * size : (c + 1) * size].reshape(nkv, rows, size)
            sbuf[c, :, :, start : start + size] = piece.astype(BF16)

    project("write", write, 0)
    project("read", read, wc)
    project("value", value, 2 * wc)
    project("gate", gate, 2 * wc + vc)

    def source(part, half, rank):
        if part == chunks:
            return saux.at[half + rank]
        return sbuf.at[part, half + rank]

    def spread_out(part, half, target, target_aux, send, recv):
        copies = []
        for off in range(1, inner):
            rank = lax.rem(place + off, inner)
            dst = target_aux.at[off - 1] if part == chunks else target.at[part, off - 1]
            copy = pltpu.make_async_remote_copy(
                src_ref=source(part, half, rank), dst_ref=dst,
                send_sem=send.at[part, off - 1], recv_sem=recv.at[part, off - 1],
                device_id={"kv": mine + rank}, device_id_type=MESH,
            )
            copy.start()
            copies.append(copy)
        return copies

    pl.semaphore_wait(barrier, nkv - 1 + ntp - 1)
    parts_order = (chunks,) + tuple(range(chunks))
    far = {p: spread_out(p, theirs, fbuf, faux, f_send, f_recv) for p in parts_order}
    near = {p: spread_out(p, mine, nbuf, naux, n_send, n_recv) for p in parts_order}
    cross = {}

    def forward(part):
        for copy in far[part]:
            copy.wait_recv()
        if part == chunks:
            total = saux[theirs + place]
            for off in range(1, inner):
                total = total + faux[off - 1]
            xsa[...] = total
            src, dst = xsa, xra
        else:
            total = sbuf[part, theirs + place].astype(F32)
            for off in range(1, inner):
                total = total + fbuf[part, off - 1].astype(F32)
            xs[part] = total.astype(BF16)
            src, dst = xs.at[part], xr.at[part]
        copy = pltpu.make_async_remote_copy(
            src_ref=src, dst_ref=dst,
            send_sem=x_send.at[part], recv_sem=x_recv.at[part],
            device_id={"kv": theirs + place}, device_id_type=MESH,
        )
        copy.start()
        cross[part] = copy

    def arrive(part):
        for copy in near[part]:
            copy.wait_recv()
        cross[part].wait_recv()

    for name in (
        "acc", "rawv", "raww", "rawr", "tapv", "tapw", "tapr", "bias", "rate", "direct",
        "prior", "extra",
    ):
        loads[name].wait()
    early = TAPS - 1
    kinds = early + TAPS

    def shifts(ref, count):
        flat = jnp.concatenate([ref[r].astype(F32) for r in range(raw_len)], axis=0)
        shape = (count * rows, raw_len * seqs)
        index, column = iota(shape, 0), iota(shape, 1)
        kind = lax.div(index, rows)
        within = lax.rem(index, rows)
        t = lax.rem(within, DRAFT)
        seq = lax.div(within, DRAFT)
        r = lax.div(column, seqs)
        begin = jnp.zeros(shape, jnp.int32)
        for s in range(seqs):
            begin = jnp.where(seq == s, acc[s], begin)
        is_early = (kind < early) & (t + kind < early) & (r == begin + t + kind)
        is_last = (kind >= early) & (r == t + kind - early)
        here = seq == lax.rem(column, seqs)
        pick = jnp.where(here & (is_early | is_last), 1.0, 0.0).astype(BF16)
        return dot(pick, flat.astype(BF16))

    def tap(taps, j):
        return taps[j : j + 1, :].astype(F32)

    def early_of(moved, taps):
        return sum(
            moved[j * rows : (j + 1) * rows] * tap(taps, j) for j in range(early)
        )

    def last_of(moved, taps):
        return silu(
            sum(
                moved[(early + j) * rows : (early + j + 1) * rows] * tap(taps, j)
                for j in range(TAPS)
            )
        )

    moved = shifts(rawv, kinds)
    early_v = early_of(moved, tapv)
    last_v = last_of(moved, tapv)
    moved = shifts(raww, kinds)
    early_w = early_of(moved, tapw)
    last_w = last_of(moved, tapw)
    early_r = early_of(shifts(rawr, early), tapr)

    square = (rows, rows)
    ri, ci = iota(square, 0), iota(square, 1)
    same = lax.div(ri, DRAFT) == lax.div(ci, DRAFT)

    def mix(mask, x):
        return dot(jnp.where(mask, 1.0, 0.0), x, precision=lax.Precision.HIGHEST)

    spread = jnp.where(
        lax.div(iota((heads, cv), 1), HEAD_DIM) == iota((heads, cv), 0), 1.0, 0.0
    ).astype(BF16)

    def expand(x):
        high, low = split(x)
        return dot(high, spread) + dot(low, spread)

    head_shape = (rows, heads)
    row_h = iota(head_shape, 0)
    rate_e = jnp.exp(rate[...])
    seq_h = lax.div(row_h, DRAFT)
    accepted = jnp.zeros(head_shape, jnp.int32)
    for s in range(seqs):
        accepted = jnp.where(seq_h == s, acc[s], accepted)
    live = jnp.where(lax.rem(row_h, DRAFT) < accepted, 1.0, 0.0)
    prior_x = jnp.concatenate([prior[s] for s in range(seqs)], axis=0)
    extra_p = jnp.concatenate([extra[s, :DRAFT] for s in range(seqs)], axis=0)
    extra_n = jnp.concatenate([extra[s, DRAFT:] for s in range(seqs)], axis=0)
    prior_step = softplus(prior_x + bias[...])
    kept = live * (extra_p - rate_e * prior_step)
    total_decay = jnp.exp(mix(same, kept))
    tail = mix(same & (ci > ri), kept)
    coefficient = expand(live * jnp.exp(tail) * prior_step)
    direct_e = expand(jnp.broadcast_to(direct[...], head_shape))
    weighted = coefficient * last_v
    row_c = lax.div(iota((rows, width), 0), DRAFT)
    for part in parts_order:
        forward(part)
    loads["state"].wait()
    for g in range(groups):
        lanes = slice(g * STATE, (g + 1) * STATE)
        for s in range(seqs):
            a = jnp.where(row_c == s, weighted[:, g * width : (g + 1) * width], 0.0)
            added = dot(a, last_w[:, lanes], ((0,), (0,)), lax.Precision.HIGHEST)
            for i in range(per_group):
                h = g * per_group + i
                decay = total_decay[s * DRAFT : s * DRAFT + 1, h : h + 1]
                new = decay * state[s, h] + added[i * HEAD_DIM : (i + 1) * HEAD_DIM]
                res_ref[s, h] = new
                high, low = split(new)
                at = slice(h * HEAD_DIM, (h + 1) * HEAD_DIM)
                s_hi[s, at] = high
                s_lo[s, at] = low

    arrive(chunks)
    aux = saux[me] + xra[...]
    for off in range(1, inner):
        aux = aux + naux[off - 1]
    inverse = lax.rsqrt(aux[:, STATE - 1 :] * (1.0 / (depth * nkv)) + EPS)
    step_pre = inverse * aux[:, :heads]
    step_now = softplus(step_pre + bias[...])
    log_decay = extra_n - rate_e * step_now
    cumulative = mix(same & (ci <= ri), log_decay)
    stack = [jnp.exp(cumulative)]
    for d in range(DRAFT):
        if d == 0:
            stack.append(step_now)
        else:
            back = same & (ci == ri - d)
            gap = cumulative - mix(back, cumulative)
            stack.append(jnp.exp(jnp.minimum(gap, 0.0)) * mix(back, step_now))
    wide = expand(jnp.concatenate(stack, axis=0))
    carry_e = wide[:rows]
    coef = [wide[(d + 1) * rows : (d + 2) * rows] for d in range(DRAFT)]

    def summed(part, start, size):
        at = slice(start, start + size)
        total = sbuf[part, me, :, at].astype(F32) + xr[part, :, at].astype(F32)
        for off in range(1, inner):
            total = total + nbuf[part, off - 1, :, at].astype(F32)
        return (inverse * total).astype(BF16).astype(F32)

    def delayed(x, d):
        if d == 0:
            return x
        keep = lax.rem(iota(x.shape, 0), DRAFT) >= d
        return jnp.where(keep, pltpu.roll(x, d, 0), 0.0)

    def conv(before, new, taps, begin):
        at = slice(begin, begin + new.shape[1])
        total = before[:, at]
        for d in range(DRAFT):
            total = total + tap(taps, TAPS - 1 - d)[:, at] * delayed(new, d)
        return silu(total)

    loads["gng"].wait()
    gathers = []
    for c in range(chunks):
        arrive(c)
        writes = conv(early_w, summed(c, 0, wc), tapw, c * wc)
        reads = conv(early_r, summed(c, wc, wc), tapr, c * wc)
        values = conv(early_v, summed(c, 2 * wc, vc), tapv, c * vc)
        opened = silu(summed(c, 2 * wc + vc, vc))
        r_hi, r_lo = split(reads)
        r_both = jnp.concatenate([r_hi, r_lo], axis=0)
        moved_writes = [delayed(writes, d) for d in range(DRAFT)]
        moved_values = [delayed(values, d) for d in range(DRAFT)]
        for k in range(gc):
            g = c * gc + k
            lanes = slice(k * STATE, (k + 1) * STATE)
            near_at = slice(k * width, (k + 1) * width)
            at = slice(g * width, (g + 1) * width)
            carried = None
            for s in range(seqs):
                both = dot(r_both[:, lanes], s_hi[s, at], ((1,), (1,)))
                low = dot(r_hi[:, lanes], s_lo[s, at], ((1,), (1,)))
                one = both[:rows] + both[rows:] + low
                carried = one if carried is None else jnp.where(row_c == s, one, carried)
            mixed = carry_e[:, at] * carried + direct_e[:, at] * values[:, near_at]
            for d in range(DRAFT):
                product = jnp.sum(
                    reads[:, lanes] * moved_writes[d][:, lanes], axis=1, keepdims=True
                )
                mixed = mixed + product * coef[d][:, at] * moved_values[d][:, near_at]
            gated = mixed * opened[:, near_at]
            scale = lax.rsqrt(
                jnp.sum(gated * gated, axis=1, keepdims=True) * (1.0 / width) + EPS
            )
            gbuf[c, me, :, near_at] = (gated * scale * gng[:, at]).astype(BF16)

        for off in range(nkv - 1, 0, -1):
            peer = lax.rem(me + off, nkv)
            copy = pltpu.make_async_remote_copy(
                src_ref=gbuf.at[c, me], dst_ref=gbuf.at[c, me],
                send_sem=gsend_sem.at[c, off - 1], recv_sem=grecv_sem.at[c, off - 1],
                device_id={"kv": peer}, device_id_type=MESH,
            )
            copy.start()
            gathers.append((c, copy))
    loads["outm"].wait()
    share = tokens // ntp
    partial = None
    for c in range(chunks):
        for k, copy in gathers:
            if k == c:
                copy.wait_recv()
        normed = gbuf[c].astype(F32).reshape(tokens, vc).astype(BF16)
        term = dot(normed, outm[c * vc : (c + 1) * vc])
        partial = term if partial is None else partial + term
    pbuf[...] = partial.reshape(ntp, share, outm.shape[1]).astype(BF16)
    parts = []
    for off in range(1, ntp):
        peer = lax.rem(my_tp + off, ntp)
        copy = pltpu.make_async_remote_copy(
            src_ref=pbuf.at[peer], dst_ref=qbuf.at[off - 1],
            send_sem=psend_sem.at[off - 1], recv_sem=precv_sem.at[off - 1],
            device_id={"tp": peer}, device_id_type=MESH,
        )
        copy.start()
        parts.append(copy)
    total = pbuf[my_tp].astype(F32)
    for off in range(1, ntp):
        parts[off - 1].wait_recv()
        total = total + qbuf[off - 1].astype(F32)
    out_ref[...] = total.astype(BF16)
    for p in parts_order:
        for copy in far[p] + near[p] + [cross[p]]:
            copy.wait_send()
    for copy in [copy for _, copy in gathers] + parts:
        copy.wait_send()


def per_device(nkv, ntp, *args):
    flat = [x.reshape(1, -1) if x.ndim == 1 and x.dtype == F32 else x for x in args]
    flat[6] = flat[6].T
    for i in (7, 8, 9):
        flat[i] = flat[i].transpose(1, 0, 2)
    tokens = args[0].shape[0]
    rows = tokens // nkv
    gate, value, write, read, step = args[2:7]
    outm = args[21]
    cv, cw = value.shape[1], write.shape[1]
    groups = cw // STATE
    chunks = 2 if groups % 2 == 0 else 1
    inner = nkv // 2
    total = (gate.shape[1] + cv + 2 * cw) // chunks
    state = args[19]
    scratch = []
    for i, x in enumerate(flat):
        space = pltpu.SMEM if i == 18 else pltpu.VMEM
        scratch.append(space(x.shape, x.dtype))
    DMA = pltpu.SemaphoreType.DMA
    scratch += [
        pltpu.VMEM((chunks, nkv, rows, total), BF16),
        pltpu.VMEM((chunks, inner - 1, rows, total), BF16),
        pltpu.VMEM((chunks, inner - 1, rows, total), BF16),
        pltpu.VMEM((chunks, rows, total), BF16),
        pltpu.VMEM((chunks, rows, total), BF16),
        pltpu.VMEM((nkv, rows, STATE), F32),
        pltpu.VMEM((inner - 1, rows, STATE), F32),
        pltpu.VMEM((inner - 1, rows, STATE), F32),
        pltpu.VMEM((rows, STATE), F32),
        pltpu.VMEM((rows, STATE), F32),
        pltpu.VMEM((chunks, nkv, rows, cv // chunks), BF16),
        pltpu.VMEM((ntp, tokens // ntp, outm.shape[1]), BF16),
        pltpu.VMEM((ntp - 1, tokens // ntp, outm.shape[1]), BF16),
        pltpu.VMEM((state.shape[0], cv, STATE), BF16),
        pltpu.VMEM((state.shape[0], cv, STATE), BF16),
        DMA((len(flat),)),
        DMA((chunks + 1, inner - 1)),
        DMA((chunks + 1, inner - 1)),
        DMA((chunks + 1, inner - 1)),
        DMA((chunks + 1, inner - 1)),
        DMA((chunks + 1,)),
        DMA((chunks + 1,)),
        DMA((chunks, nkv - 1)),
        DMA((chunks, nkv - 1)),
        DMA((ntp - 1,)),
        DMA((ntp - 1,)),
    ]
    return pl.pallas_call(
        functools.partial(body, nkv, ntp),
        out_shape=(
            pltpu.VMEM((tokens // ntp, outm.shape[1]), BF16),
            pltpu.VMEM(state.shape, F32),
        ),
        in_specs=[pl.BlockSpec(memory_space=pl.ANY)] * len(flat),
        out_specs=(
            pl.BlockSpec(memory_space=pltpu.VMEM),
            pl.BlockSpec(memory_space=pltpu.VMEM),
        ),
        scratch_shapes=scratch,
        compiler_params=pltpu.CompilerParams(collective_id=0, has_side_effects=True),
        name="mixer",
    )(*flat)


def solution(mesh):
    placed = (
        P(None, "kv"),
        P("kv"),
        P("kv", "tp"),
        P("kv", "tp"),
        P("kv", "tp"),
        P("kv", "tp"),
        P("kv", "tp"),
        P("kv", None, "tp"),
        P("kv", None, "tp"),
        P("kv", None, "tp"),
        P(None, "tp"),
        P(None, "tp"),
        P(None, "tp"),
        P("tp"),
        P("tp"),
        P("tp"),
        P("kv", None, "tp"),
        P("kv", None, "tp"),
        P("kv"),
        P("kv", "tp", None, None),
        P("tp"),
        P("tp", "kv"),
    )
    return jax.shard_map(
        functools.partial(per_device, mesh.shape["kv"], mesh.shape["tp"]),
        mesh=mesh,
        in_specs=placed,
        out_specs=(P("tp", "kv"), P("kv", "tp", None, None)),
        check_vma=False,
    )
```

```python
import functools

import jax
import jax.numpy as jnp
from jax import lax
from jax.experimental import pallas as pl
from jax.experimental.pallas import tpu as pltpu
from jax.sharding import PartitionSpec as P

HEAD_DIM = 64
STATE = 128
TAPS = 4
DRAFT = 4
EPS = 1e-06
F32 = jnp.float32
BF16 = jnp.bfloat16


def iota(shape, dim):
    return lax.broadcasted_iota(jnp.int32, shape, dim)


def silu(x):
    return x / (1.0 + jnp.exp(-x))


def softplus(x):
    return jnp.maximum(x, 0.0) + jnp.log1p(jnp.exp(-jnp.abs(x)))


def dot(a, b, dims=((1,), (0,)), precision=None):
    return lax.dot_general(
        a, b, (dims, ((), ())), preferred_element_type=F32, precision=precision
    )


def split(x):
    high = x.astype(BF16)
    return high, (x - high.astype(F32)).astype(BF16)


def body(nkv, ntp, *refs):
    (
        hid_h, gain_h, gate_h, value_h, write_h, read_h, step_h,
        rawv_h, raww_h, rawr_h, tapv_h, tapw_h, tapr_h,
        bias_h, rate_h, direct_h, prior_h, extra_h, acc_h, state_h, gng_h, outm_h,
        out_ref, res_ref,
        hid, gain, gate, value, write, read, step, rawv, raww, rawr,
        tapv, tapw, tapr, bias, rate, direct, prior, extra, acc, state, gng, outm,
        sbuf, fbuf, nbuf, xs, xr, saux, faux, naux, xsa, xra,
        gbuf, pbuf, qbuf, s_hi, s_lo,
        load_sem, f_send, f_recv, n_send, n_recv, x_send, x_recv,
        gsend_sem, grecv_sem, psend_sem, precv_sem,
    ) = refs
    me = lax.axis_index("kv")
    my_tp = lax.axis_index("tp")
    chunks, _, rows, _ = sbuf.shape
    inner = nkv // 2
    place = lax.rem(me, inner)
    mine = me - place
    theirs = inner - mine
    seqs = rawv.shape[1]
    tokens, depth = hid.shape
    heads = step.shape[0]
    cv, cw = value.shape[1], write.shape[1]
    groups = cw // STATE
    width = cv // groups
    per_group = heads // groups
    raw_len = rawv.shape[0]
    MESH = pl.DeviceIdType.MESH

    loads = {}
    order = (
        ("hid", hid_h, hid), ("gain", gain_h, gain), ("step", step_h, step),
        ("write", write_h, write), ("read", read_h, read), ("value", value_h, value),
        ("gate", gate_h, gate), ("acc", acc_h, acc), ("rawv", rawv_h, rawv),
        ("raww", raww_h, raww), ("rawr", rawr_h, rawr), ("tapv", tapv_h, tapv),
        ("tapw", tapw_h, tapw), ("tapr", tapr_h, tapr), ("bias", bias_h, bias),
        ("rate", rate_h, rate), ("direct", direct_h, direct), ("prior", prior_h, prior),
        ("extra", extra_h, extra), ("state", state_h, state), ("gng", gng_h, gng),
        ("outm", outm_h, outm),
    )
    for i, (name, src, dst) in enumerate(order):
        loads[name] = pltpu.make_async_copy(src, dst, load_sem.at[i])
        loads[name].start()

    barrier = pltpu.get_barrier_semaphore()
    for off in range(1, nkv):
        pl.semaphore_signal(
            barrier, inc=1, device_id={"kv": lax.rem(me + off, nkv)}, device_id_type=MESH
        )
    for off in range(1, ntp):
        pl.semaphore_signal(
            barrier, inc=1, device_id={"tp": lax.rem(my_tp + off, ntp)}, device_id_type=MESH
        )

    loads["hid"].wait()
    loads["gain"].wait()
    loads["step"].wait()
    floats = hid[...].astype(F32)
    squares = jnp.sum(floats * floats, axis=1, keepdims=True)
    scaled = (floats * gain[...]).astype(BF16)
    saux[...] = jnp.broadcast_to(squares, (tokens, STATE)).reshape(nkv, rows, STATE)
    saux[:, :, :heads] = dot(scaled, step[...], ((1,), (1,))).reshape(nkv, rows, heads)
    wc, vc, gc = cw // chunks, cv // chunks, groups // chunks

    def project(name, ref, start):
        loads[name].wait()
        size = ref.shape[1] // chunks
        part = dot(scaled, ref[...])
        for c in range(chunks):
            piece = part[:, c * size : (c + 1) * size].reshape(nkv, rows, size)
            sbuf[c, :, :, start : start + size] = piece.astype(BF16)

    project("write", write, 0)
    project("read", read, wc)
    project("value", value, 2 * wc)
    project("gate", gate, 2 * wc + vc)

    def source(part, half, rank):
        if part == chunks:
            return saux.at[half + rank]
        return sbuf.at[part, half + rank]

    def spread_out(part, half, target, target_aux, send, recv):
        copies = []
        for off in range(1, inner):
            rank = lax.rem(place + off, inner)
            dst = target_aux.at[off - 1] if part == chunks else target.at[part, off - 1]
            copy = pltpu.make_async_remote_copy(
                src_ref=source(part, half, rank), dst_ref=dst,
                send_sem=send.at[part, off - 1], recv_sem=recv.at[part, off - 1],
                device_id={"kv": mine + rank}, device_id_type=MESH,
            )
            copy.start()
            copies.append(copy)
        return copies

    parts_order = (chunks,) + tuple(range(chunks))
    cross = {}
    far, near = {}, {}

    def forward(part):
        for copy in far[part]:
            copy.wait_recv()
        if part == chunks:
            total = saux[theirs + place]
            for off in range(1, inner):
                total = total + faux[off - 1]
            xsa[...] = total
            src, dst = xsa, xra
        else:
            total = sbuf[part, theirs + place].astype(F32)
            for off in range(1, inner):
                total = total + fbuf[part, off - 1].astype(F32)
            xs[part] = total.astype(BF16)
            src, dst = xs.at[part], xr.at[part]
        copy = pltpu.make_async_remote_copy(
            src_ref=src, dst_ref=dst,
            send_sem=x_send.at[part], recv_sem=x_recv.at[part],
            device_id={"kv": theirs + place}, device_id_type=MESH,
        )
        copy.start()
        cross[part] = copy

    def arrive(part):
        for copy in near[part]:
            copy.wait_recv()
        cross[part].wait_recv()

    for name in (
        "acc", "rawv", "raww", "rawr", "tapv", "tapw", "tapr", "bias", "rate", "direct",
        "prior", "extra",
    ):
        loads[name].wait()
    early = TAPS - 1
    kinds = early + TAPS

    def shifts(ref, count):
        flat = jnp.concatenate([ref[r].astype(F32) for r in range(raw_len)], axis=0)
        shape = (count * rows, raw_len * seqs)
        index, column = iota(shape, 0), iota(shape, 1)
        kind = lax.div(index, rows)
        within = lax.rem(index, rows)
        t = lax.rem(within, DRAFT)
        seq = lax.div(within, DRAFT)
        r = lax.div(column, seqs)
        begin = jnp.zeros(shape, jnp.int32)
        for s in range(seqs):
            begin = jnp.where(seq == s, acc[s], begin)
        is_early = (kind < early) & (t + kind < early) & (r == begin + t + kind)
        is_last = (kind >= early) & (r == t + kind - early)
        here = seq == lax.rem(column, seqs)
        pick = jnp.where(here & (is_early | is_last), 1.0, 0.0).astype(BF16)
        return dot(pick, flat.astype(BF16))

    def tap(taps, j):
        return taps[j : j + 1, :].astype(F32)

    def early_of(moved, taps):
        return sum(
            moved[j * rows : (j + 1) * rows] * tap(taps, j) for j in range(early)
        )

    def last_of(moved, taps):
        return silu(
            sum(
                moved[(early + j) * rows : (early + j + 1) * rows] * tap(taps, j)
                for j in range(TAPS)
            )
        )

    moved = shifts(rawv, kinds)
    early_v = early_of(moved, tapv)
    last_v = last_of(moved, tapv)
    moved = shifts(raww, kinds)
    early_w = early_of(moved, tapw)
    last_w = last_of(moved, tapw)
    early_r = early_of(shifts(rawr, early), tapr)

    square = (rows, rows)
    ri, ci = iota(square, 0), iota(square, 1)
    same = lax.div(ri, DRAFT) == lax.div(ci, DRAFT)

    def mix(mask, x):
        return dot(jnp.where(mask, 1.0, 0.0), x, precision=lax.Precision.HIGHEST)

    spread = jnp.where(
        lax.div(iota((heads, cv), 1), HEAD_DIM) == iota((heads, cv), 0), 1.0, 0.0
    ).astype(BF16)

    def expand(x):
        high, low = split(x)
        return dot(high, spread) + dot(low, spread)

    head_shape = (rows, heads)
    row_h = iota(head_shape, 0)
    rate_e = jnp.exp(rate[...])
    seq_h = lax.div(row_h, DRAFT)
    accepted = jnp.zeros(head_shape, jnp.int32)
    for s in range(seqs):
        accepted = jnp.where(seq_h == s, acc[s], accepted)
    live = jnp.where(lax.rem(row_h, DRAFT) < accepted, 1.0, 0.0)
    prior_x = jnp.concatenate([prior[s] for s in range(seqs)], axis=0)
    extra_p = jnp.concatenate([extra[s, :DRAFT] for s in range(seqs)], axis=0)
    extra_n = jnp.concatenate([extra[s, DRAFT:] for s in range(seqs)], axis=0)
    prior_step = softplus(prior_x + bias[...])
    kept = live * (extra_p - rate_e * prior_step)
    total_decay = jnp.exp(mix(same, kept))
    tail = mix(same & (ci > ri), kept)
    coefficient = expand(live * jnp.exp(tail) * prior_step)
    direct_e = expand(jnp.broadcast_to(direct[...], head_shape))
    weighted = coefficient * last_v
    row_c = lax.div(iota((rows, width), 0), DRAFT)
    loads["state"].wait()
    for g in range(groups):
        lanes = slice(g * STATE, (g + 1) * STATE)
        for s in range(seqs):
            a = jnp.where(row_c == s, weighted[:, g * width : (g + 1) * width], 0.0)
            added = dot(a, last_w[:, lanes], ((0,), (0,)), lax.Precision.HIGHEST)
            for i in range(per_group):
                h = g * per_group + i
                decay = total_decay[s * DRAFT : s * DRAFT + 1, h : h + 1]
                new = decay * state[s, h] + added[i * HEAD_DIM : (i + 1) * HEAD_DIM]
                res_ref[s, h] = new
                high, low = split(new)
                at = slice(h * HEAD_DIM, (h + 1) * HEAD_DIM)
                s_hi[s, at] = high
                s_lo[s, at] = low

    pl.semaphore_wait(barrier, nkv - 1 + ntp - 1)
    far.update({p: spread_out(p, theirs, fbuf, faux, f_send, f_recv) for p in parts_order})
    near.update({p: spread_out(p, mine, nbuf, naux, n_send, n_recv) for p in parts_order})
    for part in parts_order:
        forward(part)
    arrive(chunks)
    aux = saux[me] + xra[...]
    for off in range(1, inner):
        aux = aux + naux[off - 1]
    inverse = lax.rsqrt(aux[:, STATE - 1 :] * (1.0 / (depth * nkv)) + EPS)
    step_pre = inverse * aux[:, :heads]
    step_now = softplus(step_pre + bias[...])
    log_decay = extra_n - rate_e * step_now
    cumulative = mix(same & (ci <= ri), log_decay)
    stack = [jnp.exp(cumulative)]
    for d in range(DRAFT):
        if d == 0:
            stack.append(step_now)
        else:
            back = same & (ci == ri - d)
            gap = cumulative - mix(back, cumulative)
            stack.append(jnp.exp(jnp.minimum(gap, 0.0)) * mix(back, step_now))
    wide = expand(jnp.concatenate(stack, axis=0))
    carry_e = wide[:rows]
    coef = [wide[(d + 1) * rows : (d + 2) * rows] for d in range(DRAFT)]

    def summed(part, start, size):
        at = slice(start, start + size)
        total = sbuf[part, me, :, at].astype(F32) + xr[part, :, at].astype(F32)
        for off in range(1, inner):
            total = total + nbuf[part, off - 1, :, at].astype(F32)
        return (inverse * total).astype(BF16).astype(F32)

    def delayed(x, d):
        if d == 0:
            return x
        keep = lax.rem(iota(x.shape, 0), DRAFT) >= d
        return jnp.where(keep, pltpu.roll(x, d, 0), 0.0)

    def conv(before, new, taps, begin):
        at = slice(begin, begin + new.shape[1])
        total = before[:, at]
        for d in range(DRAFT):
            total = total + tap(taps, TAPS - 1 - d)[:, at] * delayed(new, d)
        return silu(total)

    loads["gng"].wait()
    gathers = []
    for c in range(chunks):
        arrive(c)
        writes = conv(early_w, summed(c, 0, wc), tapw, c * wc)
        reads = conv(early_r, summed(c, wc, wc), tapr, c * wc)
        values = conv(early_v, summed(c, 2 * wc, vc), tapv, c * vc)
        opened = silu(summed(c, 2 * wc + vc, vc))
        r_hi, r_lo = split(reads)
        r_both = jnp.concatenate([r_hi, r_lo], axis=0)
        moved_writes = [delayed(writes, d) for d in range(DRAFT)]
        moved_values = [delayed(values, d) for d in range(DRAFT)]
        for k in range(gc):
            g = c * gc + k
            lanes = slice(k * STATE, (k + 1) * STATE)
            near_at = slice(k * width, (k + 1) * width)
            at = slice(g * width, (g + 1) * width)
            carried = None
            for s in range(seqs):
                both = dot(r_both[:, lanes], s_hi[s, at], ((1,), (1,)))
                low = dot(r_hi[:, lanes], s_lo[s, at], ((1,), (1,)))
                one = both[:rows] + both[rows:] + low
                carried = one if carried is None else jnp.where(row_c == s, one, carried)
            mixed = carry_e[:, at] * carried + direct_e[:, at] * values[:, near_at]
            for d in range(DRAFT):
                product = jnp.sum(
                    reads[:, lanes] * moved_writes[d][:, lanes], axis=1, keepdims=True
                )
                mixed = mixed + product * coef[d][:, at] * moved_values[d][:, near_at]
            gated = mixed * opened[:, near_at]
            scale = lax.rsqrt(
                jnp.sum(gated * gated, axis=1, keepdims=True) * (1.0 / width) + EPS
            )
            gbuf[c, me, :, near_at] = (gated * scale * gng[:, at]).astype(BF16)

        for off in list(range(inner, nkv)) + list(range(1, inner)):
            half = theirs if off >= inner else mine
            peer = half + lax.rem(place + off, inner)
            copy = pltpu.make_async_remote_copy(
                src_ref=gbuf.at[c, me], dst_ref=gbuf.at[c, me],
                send_sem=gsend_sem.at[c, off - 1], recv_sem=grecv_sem.at[c, off - 1],
                device_id={"kv": peer}, device_id_type=MESH,
            )
            copy.start()
            gathers.append((c, copy))
    loads["outm"].wait()
    share = tokens // ntp
    partial = None
    for c in range(chunks):
        for k, copy in gathers:
            if k == c:
                copy.wait_recv()
        normed = gbuf[c].astype(F32).reshape(tokens, vc).astype(BF16)
        term = dot(normed, outm[c * vc : (c + 1) * vc])
        partial = term if partial is None else partial + term
    pbuf[...] = partial.reshape(ntp, share, outm.shape[1]).astype(BF16)
    parts = []
    for off in range(1, ntp):
        peer = lax.rem(my_tp + off, ntp)
        copy = pltpu.make_async_remote_copy(
            src_ref=pbuf.at[peer], dst_ref=qbuf.at[off - 1],
            send_sem=psend_sem.at[off - 1], recv_sem=precv_sem.at[off - 1],
            device_id={"tp": peer}, device_id_type=MESH,
        )
        copy.start()
        parts.append(copy)
    total = pbuf[my_tp].astype(F32)
    for off in range(1, ntp):
        parts[off - 1].wait_recv()
        total = total + qbuf[off - 1].astype(F32)
    out_ref[...] = total.astype(BF16)
    for p in parts_order:
        for copy in far[p] + near[p] + [cross[p]]:
            copy.wait_send()
    for copy in [copy for _, copy in gathers] + parts:
        copy.wait_send()


def per_device(nkv, ntp, *args):
    flat = [x.reshape(1, -1) if x.ndim == 1 and x.dtype == F32 else x for x in args]
    flat[6] = flat[6].T
    for i in (7, 8, 9):
        flat[i] = flat[i].transpose(1, 0, 2)
    tokens = args[0].shape[0]
    rows = tokens // nkv
    gate, value, write, read, step = args[2:7]
    outm = args[21]
    cv, cw = value.shape[1], write.shape[1]
    groups = cw // STATE
    chunks = 2 if groups % 2 == 0 else 1
    inner = nkv // 2
    total = (gate.shape[1] + cv + 2 * cw) // chunks
    state = args[19]
    scratch = []
    for i, x in enumerate(flat):
        space = pltpu.SMEM if i == 18 else pltpu.VMEM
        scratch.append(space(x.shape, x.dtype))
    DMA = pltpu.SemaphoreType.DMA
    scratch += [
        pltpu.VMEM((chunks, nkv, rows, total), BF16),
        pltpu.VMEM((chunks, inner - 1, rows, total), BF16),
        pltpu.VMEM((chunks, inner - 1, rows, total), BF16),
        pltpu.VMEM((chunks, rows, total), BF16),
        pltpu.VMEM((chunks, rows, total), BF16),
        pltpu.VMEM((nkv, rows, STATE), F32),
        pltpu.VMEM((inner - 1, rows, STATE), F32),
        pltpu.VMEM((inner - 1, rows, STATE), F32),
        pltpu.VMEM((rows, STATE), F32),
        pltpu.VMEM((rows, STATE), F32),
        pltpu.VMEM((chunks, nkv, rows, cv // chunks), BF16),
        pltpu.VMEM((ntp, tokens // ntp, outm.shape[1]), BF16),
        pltpu.VMEM((ntp - 1, tokens // ntp, outm.shape[1]), BF16),
        pltpu.VMEM((state.shape[0], cv, STATE), BF16),
        pltpu.VMEM((state.shape[0], cv, STATE), BF16),
        DMA((len(flat),)),
        DMA((chunks + 1, inner - 1)),
        DMA((chunks + 1, inner - 1)),
        DMA((chunks + 1, inner - 1)),
        DMA((chunks + 1, inner - 1)),
        DMA((chunks + 1,)),
        DMA((chunks + 1,)),
        DMA((chunks, nkv - 1)),
        DMA((chunks, nkv - 1)),
        DMA((ntp - 1,)),
        DMA((ntp - 1,)),
    ]
    return pl.pallas_call(
        functools.partial(body, nkv, ntp),
        out_shape=(
            pltpu.VMEM((tokens // ntp, outm.shape[1]), BF16),
            pltpu.VMEM(state.shape, F32),
        ),
        in_specs=[pl.BlockSpec(memory_space=pl.ANY)] * len(flat),
        out_specs=(
            pl.BlockSpec(memory_space=pltpu.VMEM),
            pl.BlockSpec(memory_space=pltpu.VMEM),
        ),
        scratch_shapes=scratch,
        compiler_params=pltpu.CompilerParams(collective_id=0, has_side_effects=True),
        name="mixer",
    )(*flat)


def solution(mesh):
    placed = (
        P(None, "kv"),
        P("kv"),
        P("kv", "tp"),
        P("kv", "tp"),
        P("kv", "tp"),
        P("kv", "tp"),
        P("kv", "tp"),
        P("kv", None, "tp"),
        P("kv", None, "tp"),
        P("kv", None, "tp"),
        P(None, "tp"),
        P(None, "tp"),
        P(None, "tp"),
        P("tp"),
        P("tp"),
        P("tp"),
        P("kv", None, "tp"),
        P("kv", None, "tp"),
        P("kv"),
        P("kv", "tp", None, None),
        P("tp"),
        P("tp", "kv"),
    )
    return jax.shard_map(
        functools.partial(per_device, mesh.shape["kv"], mesh.shape["tp"]),
        mesh=mesh,
        in_specs=placed,
        out_specs=(P("tp", "kv"), P("kv", "tp", None, None)),
        check_vma=False,
    )
```
